32 devices in a mesh: ep: 8 (over z, y), tp: 4 (over x, core).
Axes of the slice: x: 2, y: 2, z: 4, core: 2. Of those that a mesh axis runs over, the one named last changes fastest.
Arguments:
- mixer_input: bfloat16 [4096, 2048], P('ep'), may hold values from -6 to 6
- log_forget_total: float32 [16, 4096], P('tp'), may hold values from -684 to 0, as said below
- mixer_gain: float32 [2048], replicated, may hold values from 0.1 to 1.9
- w_query: bfloat16 [2048, 1024], P(None, 'tp'), may hold values from -1 to 1
- w_key: bfloat16 [2048, 256], P(None, 'tp'), may hold values from -8 to 8
- w_value: bfloat16 [2048, 256], P(None, 'tp'), may hold values from -0.125 to 0.125
- w_output: bfloat16 [1024, 2048], replicated, may hold values from -0.1875 to 0.1875
- mixer_post_gain: float32 [2048], replicated, may hold values from 0.1 to 1.9
- expert_input: bfloat16 [2048, 2048], P('ep'), may hold values from -6 to 6
- expert_ids: int32 [2048, 2], P('ep'), may hold values from 0 to 7, all different within a row; in each aligned block of 64 rows (0 to 63, 64 to 127, ...) at most 32 rows name the same one
- route_weight: float32 [2048, 2], P('ep'), may hold values from 0.1 to 1
- expert_gain: float32 [2048], replicated, may hold values from 0.1 to 1.9
- w_gate: bfloat16 [8, 2048, 3584], P('ep', None, 'tp'), may hold values from -0.125 to 0.125
- w_up: bfloat16 [8, 2048, 3584], P('ep', None, 'tp'), may hold values from -0.125 to 0.125
- w_down: bfloat16 [8, 3584, 2048], P('ep', 'tp'), may hold values from -0.09375 to 0.09375
- expert_post_gain: float32 [2048], replicated, may hold values from 0.1 to 1.9
Outputs:
- mixer_out: bfloat16 [4096, 2048], P(('ep', 'tp'))
- expert_out: bfloat16 [2048, 2048], P(('ep', 'tp'))
The draws below stay inside these ranges and needn't reach their ends.
Inputs may be any that keep to these rules, and one draw needn't show every extreme that they name: `expert_ids`: in each aligned block of 64 tokens no expert is named by more than 32 of them. `log_forget_total`: each head's values never rise along the positions.
All inputs are finite; a program needn't handle non-finite values.
Results may differ from the reference program's by a relative error of at most 0.012.
The reference program's roundings to bfloat16 on the way count: a program that leaves them out, or rounds other values in their place, can miss the bound.
Values may be sent and summed in bfloat16 or wider, within the bound.
No kernel may reach another device: no remote copies, remote signals or barrier semaphores. Data moves between devices by JAX's collectives and lax.ppermute only.
A program may use at most 128 MiB of HBM per device.

```python
import math
import jax
import jax.numpy as jnp
import numpy as np
from jax import lax

D = 2048
QUERY_HEADS = 16
KV_HEADS = 4
HD = 64
FF = 3584
TOP_K = 2
ATT_ROWS = 512
ATTENTION_SPAN = 4096
MOE_TOKENS = 2048
EXPERTS = 8
QROWS = 64
CAPQ = 32
N_EP = 8
N_TP = 4


def draw_mixer_input(key, part):
    drawn = jax.random.normal(jax.random.fold_in(key, 7), (ATTENTION_SPAN, D), jnp.float32)
    return jnp.clip(drawn, -6.0, 6.0).astype(jnp.bfloat16)


def draw_log_forget_total(key, part):
    order = jax.random.permutation(jax.random.fold_in(key, 21), QUERY_HEADS)
    slow_count = QUERY_HEADS // 2
    slow = order < slow_count
    slow_rate = jax.random.uniform(jax.random.fold_in(key, 22), (QUERY_HEADS,), jnp.float32, 0.2, 0.8) / ATTENTION_SPAN
    fast_rate = 1.0 / jax.random.uniform(jax.random.fold_in(key, 23), (QUERY_HEADS,), jnp.float32, 30.0, 100.0)
    step_rate = jnp.where(slow, slow_rate, fast_rate)
    block_factor = jnp.exp(jax.random.uniform(jax.random.fold_in(key, 24), (ATTENTION_SPAN // ATT_ROWS, QUERY_HEADS), jnp.float32, math.log(0.4), math.log(2.5)))
    per_position = jnp.repeat(block_factor, ATT_ROWS, axis=0)
    rough = jax.random.uniform(jax.random.fold_in(key, 25), (ATTENTION_SPAN, QUERY_HEADS), jnp.float32, 0.3, 1.7)
    gate_logarithm = -step_rate[None, :] * per_position * rough
    spike_position = jax.random.randint(jax.random.fold_in(key, 26), (3,), 0, ATTENTION_SPAN)
    spike_length = jnp.log(jax.random.uniform(jax.random.fold_in(key, 27), (3, QUERY_HEADS), jnp.float32, 0.6, 0.8))
    match_count = (jnp.arange(ATTENTION_SPAN)[:, None] == spike_position[None, :]).astype(jnp.float32)
    gate_logarithm = gate_logarithm + jnp.sum(match_count[:, :, None] * spike_length[None, :, :], axis=1)
    return jnp.transpose(jnp.cumsum(gate_logarithm, axis=0))


def query_key_pair(key):
    query_w = jax.random.normal(jax.random.fold_in(key, 31), (D, QUERY_HEADS * HD), jnp.float32) * D ** (-0.5)
    key_w = jax.random.normal(jax.random.fold_in(key, 32), (D, KV_HEADS * HD), jnp.float32) * D ** (-0.5)
    return (jnp.clip(query_w, -1.0, 1.0), jnp.clip(key_w, -8.0, 8.0))


def draw_w_query(key, part):
    return query_key_pair(key)[0].astype(jnp.bfloat16)


def draw_w_key(key, part):
    return query_key_pair(key)[1].astype(jnp.bfloat16)


def level_of(key, extent, split, smallest, top_value):
    def one(axis_at, parts):
        heights = jax.random.uniform(jax.random.fold_in(jax.random.fold_in(key, 6), axis_at), (parts,), jnp.float32, smallest / len(split), top_value / len(split))
        return jnp.repeat(jnp.exp(heights), extent[axis_at] // parts).reshape((-1,) + (1,) * (len(extent) - axis_at - 1))

    loudness = one(*split[0])
    for cut in split[1:]:
        loudness = loudness * one(*cut)
    return loudness


def deal_out(rng, own, number, rows, number_of, top, bound, skew):
    order = jax.random.permutation(rng, number_of)
    heavy_load, usual = portions_of(number_of, rows * top, bound, skew, True), portions_of(number_of, rows * top, bound, skew, False)
    places = jnp.arange(number_of)

    def named(tallies, turn):
        used = int((tallies > 0).sum())
        fixed = max(1, used // 4)
        moved = fixed + (places - fixed + turn * (used - fixed)) % max(1, number_of - fixed)
        return jnp.zeros((number_of,), jnp.int32).at[order[jnp.where(places < fixed, places, moved)]].set(jnp.asarray(tallies, jnp.int32))

    tallies = jnp.where(number % 4 == 0, named(heavy_load, number // 4), named(usual, number - number // 4 - 1))
    mixed = jax.random.permutation(jax.random.fold_in(own, 3), number_of)
    source_of, receiver = mixed[0:number_of // 2 * 2:2], mixed[1:number_of // 2 * 2:2]
    margin = jnp.minimum(tallies[source_of] - 1, bound - tallies[receiver]) // 2
    margin = jnp.where((source_of == order[0]) | (receiver == order[0]) | (tallies[receiver] == 0), 0, jnp.maximum(margin, 0))
    moved = jax.random.randint(jax.random.fold_in(own, 4), (number_of // 2,), 0, 1 << 20) % (margin + 1)
    tallies = tallies.at[source_of].add(-moved).at[receiver].add(moved)
    items = jnp.searchsorted(jnp.cumsum(tallies), jnp.arange(rows * top), side="right").astype(jnp.int32)
    listing = items.reshape(top, rows).T
    listing = listing[jax.random.permutation(jax.random.fold_in(own, 1), rows)]
    turn = jax.random.randint(jax.random.fold_in(own, 2), (rows, 1), 0, top)
    return jnp.take_along_axis(listing, (jnp.arange(top)[None, :] + turn) % top, axis=1)


def portions_of(amount, total, reach, slope, full):
    weights = [(1 << 20) // math.isqrt(rank ** slope) + 1 for rank in range(1, amount + 1)]
    largest = reach if full else min(reach, max(-(-total // amount), total * weights[0] // sum(weights)))
    least = 1 if total - largest >= amount - 1 else 0
    counts, rest = [largest] + [least] * (amount - 1), total - largest - least * (amount - 1)
    while rest > 0:
        candidates = [i for i in range(1, amount) if counts[i] < largest] or [i for i in range(1, amount) if counts[i] < reach]
        mass, left = sum([weights[i] for i in candidates]), rest
        for i in candidates:
            addition = min(reach - counts[i], max(1, left * weights[i] // mass), rest)
            counts[i] = counts[i] + addition
            rest = rest - addition
    return np.array(counts)


def scatter_about(own_key, shape, scale, reach, split=(), held_as=jnp.bfloat16):
    gain = level_of(own_key, shape, split, -0.22, 0.18) if split else 1.0
    entries = jax.random.normal(own_key, shape, jnp.float32) * scale * gain
    return jnp.minimum(jnp.maximum(entries, -reach), reach).astype(held_as)


def setup_inputs(seed: int = 0) -> dict:
    seeds = jax.random.split(jax.random.key(seed), 17)
    mixer_input = draw_mixer_input(jax.random.fold_in(seeds[16], 71), 0)
    log_forget_total = draw_log_forget_total(jax.random.fold_in(seeds[16], 71), 0)
    mixer_gain = jnp.clip(1.0 + 0.18 * jax.random.normal(seeds[2], (D,), jnp.float32), 0.1, 1.9)
    w_query = draw_w_query(jax.random.fold_in(seeds[16], 71), 0)
    w_key = draw_w_key(jax.random.fold_in(seeds[16], 71), 0)
    w_value = scatter_about(seeds[5], (D, KV_HEADS * HD), D ** -0.5, 0.125, ((1, 4),))
    w_output = scatter_about(seeds[6], (QUERY_HEADS * HD, D), (QUERY_HEADS * HD) ** -0.5, 0.1875)
    mixer_post_gain = jnp.clip(1.0 + 0.18 * jax.random.normal(seeds[7], (D,), jnp.float32), 0.1, 1.9)
    expert_input = scatter_about(seeds[8], (MOE_TOKENS, D), 1.0, 6.0, ((0, 8),))
    expert_ids_keys = jax.random.split(jax.random.fold_in(seeds[9], 1), MOE_TOKENS // QROWS)
    expert_ids_turns = jax.random.permutation(jax.random.fold_in(seeds[9], 3), MOE_TOKENS // QROWS)
    expert_ids = jax.vmap(lambda own, number: deal_out(jax.random.fold_in(seeds[9], 2), own, number, QROWS, EXPERTS, TOP_K, CAPQ, 2))(expert_ids_keys, expert_ids_turns).reshape((MOE_TOKENS, TOP_K))
    route_weight = jnp.clip(jnp.exp(math.log(1.0) - 2.3025851 * jax.random.uniform(seeds[10], (MOE_TOKENS, TOP_K), jnp.float32) ** level_of(seeds[10], (MOE_TOKENS, TOP_K), ((0, 8),), -0.2, 0.2)), 0.1, 1.0)
    expert_gain = jnp.clip(1.0 + 0.18 * jax.random.normal(seeds[11], (D,), jnp.float32), 0.1, 1.9)
    w_gate = scatter_about(seeds[12], (EXPERTS, D, FF), D ** -0.5, 0.125, ((0, 8), (2, 4)))
    w_up = scatter_about(seeds[13], (EXPERTS, D, FF), D ** -0.5, 0.125, ((0, 8), (2, 4)))
    w_down = scatter_about(seeds[14], (EXPERTS, FF, D), FF ** -0.5, 0.09375, ((0, 8), (1, 4)))
    expert_post_gain = jnp.clip(1.0 + 0.18 * jax.random.normal(seeds[15], (D,), jnp.float32), 0.1, 1.9)
    return {"mixer_input": mixer_input, "log_forget_total": log_forget_total, "mixer_gain": mixer_gain, "w_query": w_query, "w_key": w_key, "w_value": w_value, "w_output": w_output, "mixer_post_gain": mixer_post_gain, "expert_input": expert_input, "expert_ids": expert_ids, "route_weight": route_weight, "expert_gain": expert_gain, "w_gate": w_gate, "w_up": w_up, "w_down": w_down, "expert_post_gain": expert_post_gain}


NEG_FILL = -1e+30
NORM_EPS = 1e-06

def norm_rows(values_in, gain_vec):
    widened = values_in.astype(jnp.float32)
    return widened * lax.rsqrt(lax.optimization_barrier(jnp.mean(widened * widened, axis=-1, keepdims=True)) + NORM_EPS) * gain_vec.astype(jnp.float32)

def rounded(values_in):
    return lax.optimization_barrier(values_in.astype(jnp.bfloat16))

def mixer_part(mixer_input, log_forget_total, mixer_gain, w_query, w_key, w_value, w_output, mixer_post_gain):
    normed = rounded(norm_rows(mixer_input, mixer_gain))
    queries = rounded(jnp.dot(normed, w_query, preferred_element_type=jnp.float32))
    key_rows = rounded(jnp.dot(normed, w_key, preferred_element_type=jnp.float32))
    value_rows = rounded(jnp.dot(normed, w_value, preferred_element_type=jnp.float32))
    group_size = QUERY_HEADS // KV_HEADS
    block_rows = math.gcd(ATTENTION_SPAN, 512)
    block_total = ATTENTION_SPAN // block_rows
    query_blocks = queries.reshape(block_total, block_rows, KV_HEADS, group_size, HD)
    key_wide = key_rows.astype(jnp.float32).reshape(ATTENTION_SPAN, KV_HEADS, HD)
    value_wide = value_rows.astype(jnp.float32).reshape(ATTENTION_SPAN, KV_HEADS, HD)
    gate_totals = log_forget_total.astype(jnp.float32).reshape(KV_HEADS, group_size, ATTENTION_SPAN)
    positions = jnp.arange(ATTENTION_SPAN, dtype=jnp.int32)
    score_scale = HD ** (-0.5)

    def one_block(operands):
        query_block, block_index = operands
        first_row = (block_index * block_rows).astype(jnp.int32)
        query_pos = first_row + jnp.arange(block_rows, dtype=jnp.int32)
        visible = positions[None, :] <= query_pos[:, None]
        outputs = []
        for head_group in range(KV_HEADS):
            group_gates = gate_totals[head_group]
            query_gate = lax.dynamic_slice_in_dim(group_gates, first_row, block_rows, 1)
            scores = jnp.einsum('qjd,kd->jqk', query_block[:, head_group].astype(jnp.float32), key_wide[:, head_group]) * score_scale
            scores = scores + query_gate[:, :, None] - group_gates[:, None, :]
            scores = jnp.where(visible[None], scores, NEG_FILL)
            row_max = lax.optimization_barrier(jnp.max(scores, axis=-1, keepdims=True))
            shifted = jnp.where(visible[None], jnp.exp(scores - row_max), 0.0)
            denominator = lax.optimization_barrier(jnp.sum(shifted, axis=-1))
            weights = rounded(shifted).astype(jnp.float32)
            numerator = jnp.einsum('jqk,kd->qjd', weights, value_wide[:, head_group])
            outputs.append(numerator / jnp.transpose(denominator)[:, :, None])
        return rounded(jnp.concatenate(outputs, axis=1).reshape(block_rows, QUERY_HEADS * HD))
    mixed_heads = lax.map(one_block, (query_blocks, jnp.arange(block_total, dtype=jnp.int32)))
    mixed_heads = mixed_heads.reshape(ATTENTION_SPAN, QUERY_HEADS * HD)
    projected = jnp.dot(mixed_heads, w_output, preferred_element_type=jnp.float32)
    return norm_rows(projected, mixer_post_gain).astype(jnp.bfloat16)

def expert_part(expert_input, expert_ids, route_weight, expert_gain, w_gate, w_up, w_down, expert_post_gain):
    normed = rounded(norm_rows(expert_input, expert_gain))
    assigned = MOE_TOKENS * TOP_K
    capacity = N_EP * N_TP * CAPQ
    group_units = FF // N_TP
    flat_ids = expert_ids.reshape(assigned)
    owners = jnp.concatenate([jnp.arange(assigned, dtype=jnp.int32) // TOP_K, jnp.full((1,), MOE_TOKENS, jnp.int32)])
    shares = jnp.concatenate([route_weight.reshape(assigned).astype(jnp.float32), jnp.zeros((1,), jnp.float32)])
    padded_rows = jnp.concatenate([normed, jnp.zeros((1, D), jnp.bfloat16)], axis=0)

    def one_expert(running, expert):
        chosen = flat_ids == expert
        slot_ranks = jnp.cumsum(chosen.astype(jnp.int32)) - 1
        slot_target = jnp.where(chosen, slot_ranks, capacity).astype(jnp.int32)
        slot_table = jnp.full((capacity,), assigned, jnp.int32).at[slot_target].set(jnp.arange(assigned, dtype=jnp.int32), mode='drop')
        token_rows = owners[slot_table]
        inputs = padded_rows[token_rows]
        gate_part = jnp.dot(inputs, w_gate[expert], preferred_element_type=jnp.float32)
        up_part = jnp.dot(inputs, w_up[expert], preferred_element_type=jnp.float32)
        hidden = rounded(jax.nn.silu(gate_part) * up_part)
        down_local = w_down[expert]
        summed = jnp.zeros((capacity, D), jnp.float32)
        for group_index in range(N_TP):
            low_unit = group_index * group_units
            group_term = jnp.dot(hidden[:, low_unit:low_unit + group_units], down_local[low_unit:low_unit + group_units], preferred_element_type=jnp.float32)
            summed = summed + rounded(group_term).astype(jnp.float32)
        expert_rows = rounded(summed).astype(jnp.float32)
        running = running.at[token_rows].add(shares[slot_table][:, None] * expert_rows, mode='drop')
        return (running, None)
    combined, _ = lax.scan(one_expert, jnp.zeros((MOE_TOKENS, D), jnp.float32), jnp.arange(EXPERTS, dtype=jnp.int32))
    return norm_rows(combined, expert_post_gain).astype(jnp.bfloat16)

def reference(mixer_input, log_forget_total, mixer_gain, w_query, w_key, w_value, w_output, mixer_post_gain, expert_input, expert_ids, route_weight, expert_gain, w_gate, w_up, w_down, expert_post_gain):
    mixer_out = mixer_part(mixer_input, log_forget_total, mixer_gain, w_query, w_key, w_value, w_output, mixer_post_gain)
    expert_out = expert_part(expert_input, expert_ids, route_weight, expert_gain, w_gate, w_up, w_down, expert_post_gain)
    return (mixer_out, expert_out)
```

```python
import jax
import jax.numpy as jnp
from jax import lax
from jax.experimental import pallas as pl
from jax.experimental.pallas import tpu as pltpu
from jax.sharding import PartitionSpec as P

HD = 64
TOP_K = 2


NEG_FILL = -1e30
NORM_EPS = 1e-06


def norm_rows(values_in, gain_vec):
    widened = values_in.astype(jnp.float32)
    return (
        widened
        * lax.rsqrt(jnp.mean(widened * widened, axis=-1, keepdims=True) + NORM_EPS)
        * gain_vec
    )


def shift_pairs(count, step, wrap):
    return [(k, (k + step) % count) for k in range(count) if wrap or 0 <= k + step < count]


def flip(values_in, bit):
    count = lax.axis_size("tp")
    return lax.ppermute(values_in, "tp", [(k, k ^ bit) for k in range(count)])


def attention_kernel(rank_ref, query_ref, kv_ref, gate_ref, out_ref, wide_ref, max_ref, acc_ref):
    rows = query_ref.shape[0]
    heads = query_ref.shape[1] // HD
    kv_heads = kv_ref.shape[0]
    group = heads // kv_heads
    rank = rank_ref[0]
    low_half = lax.broadcasted_iota(jnp.int32, (rows, 2 * HD), 1) < HD
    for h in range(heads):
        one = query_ref[:, h * HD : (h + 1) * HD] * jnp.asarray(HD**-0.5, jnp.bfloat16)
        wide_ref[h] = jnp.concatenate([one, jnp.zeros_like(one)], axis=1)

    def scores_of(h, kv_block, gate_block):
        scores = lax.dot_general(
            wide_ref[h], kv_block, (((1,), (1,)), ((), ())), preferred_element_type=jnp.float32
        )
        return scores - gate_block[h : h + 1, :]

    def block(step, first):
        gate_block = gate_ref[rank - step]
        for g in range(kv_heads):
            kv_block = kv_ref[g, pl.ds(pl.multiple_of(step * rows, rows), rows), :]
            one_value = jnp.where(low_half, jnp.ones_like(kv_block), kv_block)
            for h in range(g * group, (g + 1) * group):
                scores = scores_of(h, kv_block, gate_block)
                if first:
                    visible = lax.broadcasted_iota(
                        jnp.int32, (rows, rows), 1
                    ) <= lax.broadcasted_iota(jnp.int32, (rows, rows), 0)
                    scores = jnp.where(visible, scores, NEG_FILL)
                    new_max = jnp.max(scores, axis=1, keepdims=True)
                else:
                    prior = max_ref[h][:, :1]
                    new_max = jnp.maximum(prior, jnp.max(scores, axis=1, keepdims=True))
                shifted = jnp.exp(scores - new_max).astype(jnp.bfloat16)
                term = jnp.dot(shifted, one_value, preferred_element_type=jnp.float32)
                if first:
                    acc_ref[h] = term
                else:
                    acc_ref[h] = acc_ref[h] * jnp.exp(prior - new_max) + term
                max_ref[h] = jnp.broadcast_to(new_max, (rows, 2 * HD))

    block(0, True)

    def loop_body(step, carry):
        block(step, False)
        return carry

    lax.fori_loop(1, rank + 1, loop_body, 0)
    for h in range(heads):
        total = acc_ref[h]
        out_ref[:, h * HD : (h + 1) * HD] = (total[:, HD:] / total[:, :HD]).astype(jnp.bfloat16)


def attend(rank, queries, kv_all, gates):
    rows = queries.shape[0]
    heads = queries.shape[1] // HD
    vmem = pl.BlockSpec(memory_space=pltpu.VMEM)
    return pl.pallas_call(
        attention_kernel,
        out_shape=jax.ShapeDtypeStruct(queries.shape, jnp.bfloat16),
        in_specs=[pl.BlockSpec(memory_space=pltpu.SMEM), vmem, vmem, vmem],
        out_specs=vmem,
        scratch_shapes=[
            pltpu.VMEM((heads, rows, 2 * HD), jnp.bfloat16),
            pltpu.VMEM((heads, rows, 2 * HD), jnp.float32),
            pltpu.VMEM((heads, rows, 2 * HD), jnp.float32),
        ],
        name="attend",
    )(rank.reshape(1), queries, kv_all, gates)


def mixer_start(mixer_input, log_forget_total, mixer_gain, w_query, w_key, w_value):
    row_count = mixer_input.shape[0]
    ranks = lax.axis_size("ep")
    head_local = w_query.shape[1] // HD
    kv_local = w_key.shape[1] // HD
    normed = norm_rows(mixer_input, mixer_gain).astype(jnp.bfloat16)
    key_rows = jnp.dot(normed, w_key, preferred_element_type=jnp.float32).astype(jnp.bfloat16)
    value_rows = jnp.dot(normed, w_value, preferred_element_type=jnp.float32).astype(jnp.bfloat16)
    own = jnp.concatenate(
        [
            key_rows.reshape(row_count, kv_local, HD),
            value_rows.reshape(row_count, kv_local, HD),
        ],
        axis=2,
    )
    own = jnp.transpose(own, (1, 0, 2))
    queries = jnp.dot(normed, w_query, preferred_element_type=jnp.float32).astype(jnp.bfloat16)
    gates = jnp.transpose(log_forget_total.reshape(head_local, ranks, row_count), (1, 0, 2))
    return own, queries, gates


def gather_kv(own):
    ranks = lax.axis_size("ep")
    pieces = [own]
    for step in range(1, ranks):
        pieces.append(lax.ppermute(own, "ep", shift_pairs(ranks, step, False)))
    return jnp.concatenate(pieces, axis=1)


def mixer_end(mixed_heads, w_output, mixer_post_gain):
    quarters = lax.axis_size("tp")
    mine = lax.axis_index("tp")
    rows = mixed_heads.shape[0] // quarters
    cut = mixed_heads.reshape(quarters, rows, mixed_heads.shape[1])
    pieces = []
    for bit in range(quarters):
        piece = lax.dynamic_index_in_dim(cut, mine ^ bit, 0, keepdims=False)
        pieces.append(flip(piece, bit) if bit else piece)
    stacked = jnp.stack(pieces)
    by_rows = jnp.concatenate(
        [
            lax.dynamic_index_in_dim(stacked, mine ^ source, 0, keepdims=False)
            for source in range(quarters)
        ],
        axis=1,
    )
    projected = jnp.dot(by_rows, w_output, preferred_element_type=jnp.float32)
    return norm_rows(projected, mixer_post_gain).astype(jnp.bfloat16)


def route(expert_input, expert_ids, route_weight, expert_gain):
    quarters = lax.axis_size("tp")
    experts = lax.axis_size("ep")
    quarter_rows = expert_input.shape[0] // quarters
    capacity = 2 * TOP_K * quarter_rows // experts
    first = lax.axis_index("tp") * quarter_rows
    own_rows = lax.dynamic_slice_in_dim(expert_input, first, quarter_rows, 0)
    own_ids = lax.dynamic_slice_in_dim(expert_ids, first, quarter_rows, 0)
    own_weight = lax.dynamic_slice_in_dim(route_weight, first, quarter_rows, 0)
    normed = norm_rows(own_rows, expert_gain).astype(jnp.bfloat16)
    named = (lax.axis_index("ep") + jnp.arange(experts, dtype=jnp.int32)) % experts
    chosen = own_ids[:, :, None] == named[None, None, :]
    matches = jnp.any(chosen, axis=1)
    weights = jnp.sum(jnp.where(chosen, own_weight[:, :, None], 0.0), axis=1)
    position = jnp.arange(quarter_rows, dtype=jnp.int32)
    before = (position[None, :] < position[:, None]).astype(jnp.bfloat16)
    ranks = jnp.dot(before, matches.astype(jnp.bfloat16), preferred_element_type=jnp.float32)
    ranks = jnp.where(matches, ranks.astype(jnp.int32), -1)
    placed = ranks[:, :, None] == jnp.arange(capacity, dtype=jnp.int32)[None, None, :]
    share = jnp.where(placed, weights[:, :, None], 0.0).reshape(quarter_rows, experts * capacity)
    placed = placed.reshape(quarter_rows, experts * capacity).astype(jnp.bfloat16)
    outgoing = lax.dot_general(
        placed, normed, (((0,), (0,)), ((), ())), preferred_element_type=jnp.float32
    ).astype(jnp.bfloat16)
    return outgoing, share, capacity


def exchange(rows, capacity, sign):
    experts = lax.axis_size("ep")
    pieces = [rows[:capacity]]
    for step in range(1, experts):
        piece = rows[step * capacity : (step + 1) * capacity]
        pieces.append(lax.ppermute(piece, "ep", shift_pairs(experts, sign * step, True)))
    return jnp.concatenate(pieces, axis=0)


def expert_rows_of(rows, gate_local, up_local, down_local):
    gate_part = jnp.dot(rows, gate_local, preferred_element_type=jnp.float32)
    up_part = jnp.dot(rows, up_local, preferred_element_type=jnp.float32)
    hidden = (jax.nn.silu(gate_part) * up_part).astype(jnp.bfloat16)
    return jnp.dot(hidden, down_local, preferred_element_type=jnp.float32).astype(jnp.bfloat16)


def combine(returned, share, expert_post_gain):
    high = lax.reduce_precision(share, 8, 7)
    low = lax.reduce_precision(share - high, 8, 7)
    combined = jnp.dot(
        high.astype(jnp.bfloat16), returned, preferred_element_type=jnp.float32
    ) + jnp.dot(low.astype(jnp.bfloat16), returned, preferred_element_type=jnp.float32)
    return norm_rows(combined, expert_post_gain).astype(jnp.bfloat16)


def per_device(
    mixer_input,
    log_forget_total,
    mixer_gain,
    w_query,
    w_key,
    w_value,
    w_output,
    mixer_post_gain,
    expert_input,
    expert_ids,
    route_weight,
    expert_gain,
    w_gate,
    w_up,
    w_down,
    expert_post_gain,
):
    outgoing, share, capacity = route(expert_input, expert_ids, route_weight, expert_gain)
    own_kv, queries, gates = mixer_start(
        mixer_input, log_forget_total, mixer_gain, w_query, w_key, w_value
    )
    arrived = exchange(outgoing, capacity, 1)
    kv_all = gather_kv(own_kv)
    bits = []
    bit = 1
    while bit < lax.axis_size("tp"):
        bits.append(bit)
        bit *= 2
    rows_of = {0: arrived}
    for bit in reversed(bits):
        for held in list(rows_of):
            rows_of[held | bit] = flip(rows_of[held], bit)
    mixed_heads = attend(lax.axis_index("ep"), queries, kv_all, gates)
    near = jnp.concatenate([rows_of[0], rows_of[1]], axis=0)
    far = jnp.concatenate([rows_of[2], rows_of[3]], axis=0)
    slots = arrived.shape[0]
    near_terms = expert_rows_of(near, w_gate[0], w_up[0], w_down[0])
    far_terms = expert_rows_of(far, w_gate[0], w_up[0], w_down[0])
    far_got = flip(far_terms[slots:], 1)
    near_got = flip(near_terms[slots:], 1)
    far_sum = far_terms[:slots].astype(jnp.float32) + far_got.astype(jnp.float32)
    crossed = flip(far_sum.astype(jnp.bfloat16), 2)
    near_sum = near_terms[:slots].astype(jnp.float32) + near_got.astype(jnp.float32)
    results = (near_sum + crossed.astype(jnp.float32)).astype(jnp.bfloat16)
    mixer_out = mixer_end(mixed_heads, w_output, mixer_post_gain)
    returned = exchange(results, capacity, -1)
    expert_out = combine(returned, share, expert_post_gain)
    return (mixer_out, expert_out)


def solution(mesh):
    placed = (
        P("ep", None),
        P("tp", None),
        P(),
        P(None, "tp"),
        P(None, "tp"),
        P(None, "tp"),
        P(),
        P(),
        P("ep", None),
        P("ep", None),
        P("ep", None),
        P(),
        P("ep", None, "tp"),
        P("ep", None, "tp"),
        P("ep", "tp", None),
        P(),
    )
    return jax.shard_map(
        per_device,
        mesh=mesh,
        in_specs=placed,
        out_specs=(P(("ep", "tp"), None), P(("ep", "tp"), None)),
        check_vma=False,
    )
```

```python
import functools

import jax
import jax.numpy as jnp
from jax import lax
from jax.experimental import pallas as pl
from jax.experimental.pallas import tpu as pltpu
from jax.sharding import PartitionSpec as P

HD = 64
TOP_K = 2


NEG_FILL = -1e30
NORM_EPS = 1e-06


def norm_rows(values_in, gain_vec):
    widened = values_in.astype(jnp.float32)
    return (
        widened
        * lax.rsqrt(jnp.mean(widened * widened, axis=-1, keepdims=True) + NORM_EPS)
        * gain_vec
    )


def shift_pairs(count, step, wrap):
    return [(k, (k + step) % count) for k in range(count) if wrap or 0 <= k + step < count]


def flip(values_in, bit):
    count = lax.axis_size("tp")
    return lax.ppermute(values_in, "tp", [(k, k ^ bit) for k in range(count)])


def attention_kernel(
    first_head, rank_ref, query_ref, kv_ref, gate_ref, out_ref, wide_ref, max_ref, acc_ref
):
    rows = query_ref.shape[0]
    heads = out_ref.shape[1] // HD
    group = query_ref.shape[1] // HD // kv_ref.shape[0]
    planes = kv_ref.shape[1] // rows // 2
    rank = rank_ref[0]
    low_half = lax.broadcasted_iota(jnp.int32, (rows, 2 * HD), 1) < HD
    for h in range(heads):
        at = (first_head + h) * HD
        one = query_ref[:, at : at + HD] * jnp.asarray(HD**-0.5, jnp.bfloat16)
        wide_ref[h] = jnp.concatenate([one, jnp.zeros_like(one)], axis=1)

    def block(slot, owner, first):
        gate_block = gate_ref[owner]
        for h in range(heads):
            head = first_head + h
            kv_block = kv_ref[head // group, pl.ds(pl.multiple_of(slot * rows, rows), rows), :]
            one_value = jnp.where(low_half, jnp.ones_like(kv_block), kv_block)
            scores = lax.dot_general(
                wide_ref[h], kv_block, (((1,), (1,)), ((), ())), preferred_element_type=jnp.float32
            )
            scores = scores - gate_block[head : head + 1, :]
            if first:
                visible = lax.broadcasted_iota(
                    jnp.int32, (rows, rows), 1
                ) <= lax.broadcasted_iota(jnp.int32, (rows, rows), 0)
                scores = jnp.where(visible, scores, NEG_FILL)
                new_max = jnp.max(scores, axis=1, keepdims=True)
            else:
                prior = max_ref[h][:, :1]
                new_max = jnp.maximum(prior, jnp.max(scores, axis=1, keepdims=True))
            shifted = jnp.exp(scores - new_max).astype(jnp.bfloat16)
            term = jnp.dot(shifted, one_value, preferred_element_type=jnp.float32)
            if first:
                acc_ref[h] = term
            else:
                acc_ref[h] = acc_ref[h] * jnp.exp(prior - new_max) + term
            max_ref[h] = jnp.broadcast_to(new_max, (rows, 2 * HD))

    block(0, rank, True)
    plane = rank // 2
    odd = rank % 2

    def loop_body(step, carry):
        same = step < plane
        back = jnp.where(same, step + 1, step - plane + 1 - odd)
        owner = jnp.where(same, rank, rank + 1 - 2 * odd) - 2 * back
        block(jnp.where(same, back, planes + back), owner, False)
        return carry

    lax.fori_loop(0, 2 * plane + odd, loop_body, 0)
    for h in range(heads):
        total = acc_ref[h]
        out_ref[:, h * HD : (h + 1) * HD] = (total[:, HD:] / total[:, :HD]).astype(jnp.bfloat16)


def attend(rank, queries, kv_all, gates, first_head, heads):
    rows = queries.shape[0]
    vmem = pl.BlockSpec(memory_space=pltpu.VMEM)
    pairs = rows * kv_all.shape[1] * heads
    return pl.pallas_call(
        functools.partial(attention_kernel, first_head),
        out_shape=jax.ShapeDtypeStruct((rows, heads * HD), jnp.bfloat16),
        in_specs=[pl.BlockSpec(memory_space=pltpu.SMEM), vmem, vmem, vmem],
        out_specs=vmem,
        scratch_shapes=[
            pltpu.VMEM((heads, rows, 2 * HD), jnp.bfloat16),
            pltpu.VMEM((heads, rows, 2 * HD), jnp.float32),
            pltpu.VMEM((heads, rows, 2 * HD), jnp.float32),
        ],
        cost_estimate=pl.CostEstimate(
            flops=pairs * 16 * HD, transcendentals=pairs, bytes_accessed=kv_all.size * 4
        ),
        name="attend",
    )(rank.reshape(1), queries, kv_all, gates)


def mixer_start(mixer_input, log_forget_total, mixer_gain, w_query, w_key, w_value):
    row_count = mixer_input.shape[0]
    ranks = lax.axis_size("ep")
    head_local = w_query.shape[1] // HD
    kv_local = w_key.shape[1] // HD
    normed = norm_rows(mixer_input, mixer_gain).astype(jnp.bfloat16)
    key_rows = jnp.dot(normed, w_key, preferred_element_type=jnp.float32).astype(jnp.bfloat16)
    value_rows = jnp.dot(normed, w_value, preferred_element_type=jnp.float32).astype(jnp.bfloat16)
    own = jnp.concatenate(
        [
            key_rows.reshape(row_count, kv_local, HD),
            value_rows.reshape(row_count, kv_local, HD),
        ],
        axis=2,
    )
    own = jnp.transpose(own, (1, 0, 2))
    queries = jnp.dot(normed, w_query, preferred_element_type=jnp.float32).astype(jnp.bfloat16)
    gates = jnp.transpose(log_forget_total.reshape(head_local, ranks, row_count), (1, 0, 2))
    return own, queries, gates


def gather_kv(own):
    ranks = lax.axis_size("ep")
    swap = [(k, k ^ 1) for k in range(ranks)]
    pieces = [own]
    for _ in range(1, ranks // 2):
        pieces.append(lax.ppermute(pieces[-1], "ep", shift_pairs(ranks, 2, False)))
    own_other = lax.ppermute(own, "ep", swap)
    earlier = jnp.concatenate(pieces[1:], axis=1)
    earlier_other = lax.ppermute(earlier, "ep", swap)
    return jnp.concatenate([own, earlier, own_other, earlier_other], axis=1)


def mixer_end(mixed_heads, w_output, mixer_post_gain):
    quarters = lax.axis_size("tp")
    mine = lax.axis_index("tp")
    rows = mixed_heads.shape[0] // quarters
    cut = mixed_heads.reshape(quarters, rows, mixed_heads.shape[1])
    pieces = []
    for bit in range(quarters):
        piece = lax.dynamic_index_in_dim(cut, mine ^ bit, 0, keepdims=False)
        pieces.append(flip(piece, bit) if bit else piece)
    stacked = jnp.stack(pieces)
    by_rows = jnp.concatenate(
        [
            lax.dynamic_index_in_dim(stacked, mine ^ source, 0, keepdims=False)
            for source in range(quarters)
        ],
        axis=1,
    )
    projected = jnp.dot(by_rows, w_output, preferred_element_type=jnp.float32)
    return norm_rows(projected, mixer_post_gain).astype(jnp.bfloat16)


def route(expert_input, expert_ids, route_weight, expert_gain):
    quarters = lax.axis_size("tp")
    experts = lax.axis_size("ep")
    quarter_rows = expert_input.shape[0] // quarters
    capacity = 2 * TOP_K * quarter_rows // experts
    first = lax.axis_index("tp") * quarter_rows
    own_rows = lax.dynamic_slice_in_dim(expert_input, first, quarter_rows, 0)
    own_ids = lax.dynamic_slice_in_dim(expert_ids, first, quarter_rows, 0)
    own_weight = lax.dynamic_slice_in_dim(route_weight, first, quarter_rows, 0)
    normed = norm_rows(own_rows, expert_gain).astype(jnp.bfloat16)
    named = (lax.axis_index("ep") + jnp.arange(experts, dtype=jnp.int32)) % experts
    chosen = own_ids[:, :, None] == named[None, None, :]
    matches = jnp.any(chosen, axis=1)
    weights = jnp.sum(jnp.where(chosen, own_weight[:, :, None], 0.0), axis=1)
    position = jnp.arange(quarter_rows, dtype=jnp.int32)
    before = (position[None, :] < position[:, None]).astype(jnp.bfloat16)
    ranks = jnp.dot(before, matches.astype(jnp.bfloat16), preferred_element_type=jnp.float32)
    ranks = jnp.where(matches, ranks.astype(jnp.int32), -1)
    placed = ranks[:, :, None] == jnp.arange(capacity, dtype=jnp.int32)[None, None, :]
    share = jnp.where(placed, weights[:, :, None], 0.0).reshape(quarter_rows, experts * capacity)
    placed = placed.reshape(quarter_rows, experts * capacity).astype(jnp.bfloat16)
    outgoing = lax.dot_general(
        placed, normed, (((0,), (0,)), ((), ())), preferred_element_type=jnp.float32
    ).astype(jnp.bfloat16)
    return outgoing, share, capacity


def exchange(rows, capacity, sign):
    experts = lax.axis_size("ep")
    pieces = [rows[:capacity]]
    for step in range(1, experts):
        piece = rows[step * capacity : (step + 1) * capacity]
        pieces.append(lax.ppermute(piece, "ep", shift_pairs(experts, sign * step, True)))
    return jnp.concatenate(pieces, axis=0)


def expert_rows_of(rows, gate_local, up_local, down_local):
    gate_part = jnp.dot(rows, gate_local, preferred_element_type=jnp.float32)
    up_part = jnp.dot(rows, up_local, preferred_element_type=jnp.float32)
    hidden = (jax.nn.silu(gate_part) * up_part).astype(jnp.bfloat16)
    half = rows.shape[0] // 2
    return [
        jnp.dot(part, down_local, preferred_element_type=jnp.float32).astype(jnp.bfloat16)
        for part in (hidden[half:], hidden[:half])
    ]


def combine(returned, share, expert_post_gain):
    high = lax.reduce_precision(share, 8, 7)
    low = lax.reduce_precision(share - high, 8, 7)
    combined = jnp.dot(
        high.astype(jnp.bfloat16), returned, preferred_element_type=jnp.float32
    ) + jnp.dot(low.astype(jnp.bfloat16), returned, preferred_element_type=jnp.float32)
    return norm_rows(combined, expert_post_gain).astype(jnp.bfloat16)


def per_device(
    mixer_input,
    log_forget_total,
    mixer_gain,
    w_query,
    w_key,
    w_value,
    w_output,
    mixer_post_gain,
    expert_input,
    expert_ids,
    route_weight,
    expert_gain,
    w_gate,
    w_up,
    w_down,
    expert_post_gain,
):
    own_kv, queries, gates = mixer_start(
        mixer_input, log_forget_total, mixer_gain, w_query, w_key, w_value
    )
    kv_all = gather_kv(own_kv)
    outgoing, share, capacity = route(expert_input, expert_ids, route_weight, expert_gain)
    arrived = exchange(outgoing, capacity, 1)
    rank = lax.axis_index("ep")
    heads = queries.shape[1] // HD
    half = heads // 2
    rows_0 = arrived
    rows_2 = flip(arrived, 2)
    rows_1 = flip(arrived, 1)
    mixed_low = attend(rank, queries, kv_all, gates, 0, half)
    near = jnp.concatenate([rows_0, rows_1], axis=0)
    near_1, near_0 = expert_rows_of(near, w_gate[0], w_up[0], w_down[0])
    near_got = flip(near_1, 1)
    rows_3 = flip(rows_2, 1)
    far = jnp.concatenate([rows_2, rows_3], axis=0)
    far_3, far_2 = expert_rows_of(far, w_gate[0], w_up[0], w_down[0])
    far_got = flip(far_3, 1)
    far_sum = far_2.astype(jnp.float32) + far_got.astype(jnp.float32)
    far_sum = far_sum.astype(jnp.bfloat16)
    late_queries, far_sum = lax.optimization_barrier((queries, far_sum))
    crossed = flip(far_sum, 2)
    mixed_high = attend(rank, late_queries, kv_all, gates, half, heads - half)
    near_sum = near_0.astype(jnp.float32) + near_got.astype(jnp.float32)
    results = (near_sum + crossed.astype(jnp.float32)).astype(jnp.bfloat16)
    mixed_heads = jnp.concatenate([mixed_low, mixed_high], axis=1)
    mixer_out = mixer_end(mixed_heads, w_output, mixer_post_gain)
    returned = exchange(results, capacity, -1)
    expert_out = combine(returned, share, expert_post_gain)
    return (mixer_out, expert_out)


def solution(mesh):
    placed = (
        P("ep", None),
        P("tp", None),
        P(),
        P(None, "tp"),
        P(None, "tp"),
        P(None, "tp"),
        P(),
        P(),
        P("ep", None),
        P("ep", None),
        P("ep", None),
        P(),
        P("ep", None, "tp"),
        P("ep", None, "tp"),
        P("ep", "tp", None),
        P(),
    )
    return jax.shard_map(
        per_device,
        mesh=mesh,
        in_specs=placed,
        out_specs=(P(("ep", "tp"), None), P(("ep", "tp"), None)),
        check_vma=False,
    )
```
